32 devices in a mesh: sp: 16 (over z, x, core), tp: 2 (over y).
Axes of the slice: x: 2, y: 2, z: 4, core: 2. Of those that a mesh axis runs over, the one named last changes fastest.
Arguments:
- stream: bfloat16 [2048, 16384], P('tp', 'sp'), may hold values from -12 to 12
- norm_gain: float32 [2, 2048], P(None, 'tp'), may hold values from 0.1 to 1.9
- in_weight: bfloat16 [2, 2048, 1024], P(None, 'sp', 'tp'), may hold values from -0.125 to 0.125
- out_weight: bfloat16 [2, 1024, 2048], P(None, 'tp', 'sp'), may hold values from -0.1875 to 0.1875
- docs: int32 [16384], P('sp'), may hold values from 0 to 3, never falling along the last dimension, each value on 1 to 8192 neighbouring positions
Outputs:
- mixed_out: bfloat16 [2048, 16384], P('tp', 'sp')
The draws below stay inside these ranges and needn't reach their ends.
Inputs may be any that keep to these rules, and one draw needn't show every extreme that they name: `docs`: numbers never fall along the positions and start at 0; a document spans at most 8192 positions.
All inputs are finite; a program needn't handle non-finite values.
Results may differ from the reference program's by a relative error of at most 0.0095.
Values may be sent and summed in bfloat16 or wider, within the bound.
A program may use at most 64 MiB of HBM per device.

```python
import math
import jax
import jax.numpy as jnp
import numpy as np
from jax import lax

D = 2048
PW = 1024
GROUPS = 4
WIDEST = 16
LAYERS = 2
TOKENS = 16384
DOCS = 4
DOC_MOST = 8192


def draw_stream(key, part):
    base_key, scale_key = jax.random.split(key)
    band_rows = D // 16
    base_draw = jnp.clip(jax.random.normal(base_key, (D, TOKENS), jnp.float32), -4.0, 4.0)
    levels = jnp.exp(jax.random.uniform(scale_key, (16, 1, 1), jnp.float32, jnp.log(0.3), jnp.log(3.0)))
    shaped = base_draw.reshape(16, band_rows, TOKENS) * levels
    return shaped.reshape(D, TOKENS).astype(jnp.bfloat16)


def steps_of(rng, shape, shards, low, high):
    factor_of, own = 1.0, jax.random.fold_in(rng, 6)
    for dim, shards_of in shards:
        steps = jnp.exp(jax.random.uniform(jax.random.fold_in(own, dim), (shards_of,), jnp.float32, low / len(shards), high / len(shards)))
        factor_of = factor_of * jnp.repeat(steps, shape[dim] // shards_of).reshape([-1 if axis == dim else 1 for axis in range(len(shape))])
    return factor_of


def split_up(amount, total, bound, skew):
    loads = [(1 << 20) // math.isqrt(grade ** skew) + 1 for grade in range(2, amount + 1)]
    rest, counts = total - bound - (amount - 1), [1] * (amount - 1)
    while rest > 0:
        candidates = [i for i in range(amount - 1) if counts[i] < bound]
        pool, left = sum([loads[i] for i in candidates]), rest
        for i in candidates:
            more = min(bound - counts[i], max(1, left * loads[i] // pool), rest)
            counts[i] = counts[i] + more
            rest = rest - more
    return np.array([bound] + counts)


def ragged(stream_key, count, total, limit, lean):
    if count == 2:
        one = jax.random.randint(stream_key, (), max(1, total - limit), min(limit, total - 1) + 1)
        return jnp.stack([one, total - one])
    lengths = jnp.asarray(split_up(count, total, limit, lean), jnp.int32)
    twos = (count - 1) // 2
    giver, taker = lengths[1:1 + 2 * twos:2], lengths[2:2 + 2 * twos:2]
    slack = jnp.minimum(giver - 1, limit - taker)
    moved = jax.random.randint(jax.random.fold_in(stream_key, 1), (twos,), 0, 1 << 20) % (slack + 1)
    lengths = lengths.at[1:1 + 2 * twos:2].set(giver - moved).at[2:2 + 2 * twos:2].set(taker + moved)
    return lengths[jax.random.permutation(jax.random.fold_in(stream_key, 2), count)]


def noise(stream_key, shape, scale, limit, cuts=(), kind=jnp.bfloat16):
    drawn = jax.random.normal(stream_key, shape, jnp.float32) * scale
    if len(cuts) > 0:
        drawn = steps_of(stream_key, shape, cuts, -0.22, 0.18) * drawn
    return jnp.clip(drawn, min=-limit, max=limit).astype(kind)


def setup_inputs(seed: int = 0) -> dict:
    streams_of = jax.random.split(jax.random.key(seed), 6)
    return {
        "stream": draw_stream(jax.random.fold_in(streams_of[5], 71), 0),
        "norm_gain": jnp.clip(1.0 + 0.18 * jax.random.normal(streams_of[1], (LAYERS, D), jnp.float32), 0.1, 1.9),
        "in_weight": noise(streams_of[2], (LAYERS, D, PW), D ** -0.5, 0.125, ((1, 16), (2, 2))),
        "out_weight": noise(streams_of[3], (LAYERS, PW, D), PW ** -0.5, 0.1875, ((1, 2), (2, 16))),
        "docs": jnp.searchsorted(jnp.cumsum(ragged(streams_of[4], DOCS, TOKENS, DOC_MOST, 1)), jnp.arange(TOKENS), side="right").astype(jnp.int32),
    }


def trailing_pool(values, docs, widths):
    length = values.shape[1]
    reach_back = WIDEST - 1
    extended = jnp.pad(values.astype(jnp.float32), ((0, 0), (reach_back, 0)))
    ext_docs = jnp.pad(docs + 1, (reach_back, 0))
    marker = docs + 1
    window_sum = jnp.zeros(values.shape, jnp.float32)
    members = jnp.zeros(values.shape, jnp.float32)
    for lag_step in range(WIDEST):
        lower_edge = reach_back - lag_step
        shifted = extended[:, lower_edge:lower_edge + length]
        same_doc = ext_docs[lower_edge:lower_edge + length] == marker
        inside = jnp.logical_and(same_doc[None, :], lag_step < widths[:, None])
        window_sum = window_sum + jnp.where(inside, shifted, jnp.float32(0.0))
        members = members + inside.astype(jnp.float32)
    return window_sum / members - values.astype(jnp.float32)

def reference(stream, norm_gain, in_weight, out_weight, docs):
    channel = lax.iota(jnp.int32, PW)
    widths = jnp.left_shift(jnp.int32(2), channel // (PW // GROUPS))
    residual = stream.astype(jnp.float32)
    for layer_idx in range(LAYERS):
        mean_square = lax.optimization_barrier(jnp.mean(residual * residual, axis=0))
        scaled = residual * lax.rsqrt(mean_square + 1e-06)[None, :] * norm_gain[layer_idx].astype(jnp.float32)[:, None]
        normed = scaled.astype(jnp.bfloat16)
        pool_in = jnp.dot(in_weight[layer_idx].T, normed, preferred_element_type=jnp.float32).astype(jnp.bfloat16)
        pooled = trailing_pool(pool_in, docs, widths).astype(jnp.bfloat16)
        residual = residual + jnp.dot(out_weight[layer_idx].T, pooled, preferred_element_type=jnp.float32)
    return residual.astype(jnp.bfloat16)
```

```python
import jax
import jax.numpy as jnp
from jax import lax
from jax.experimental import pallas as pl
from jax.experimental.pallas import tpu as pltpu
from jax.sharding import PartitionSpec as P
import functools

D = 2048
PW = 1024
GROUPS = 4
WIDEST = 16
LAYERS = 2


contract_rows = (((0,), (0,)), ((), ()))


def passed_along(block, axis, distance):
    devices = range(lax.axis_size(axis))
    route = [(i - distance, i) for i in devices if i - distance in devices]
    return lax.ppermute(block, axis, route)


def trailing_pool(values, docs_own, edge_values, edge_docs, widths):
    length = values.shape[1]
    reach_back = WIDEST - 1
    extended = jnp.concatenate([edge_values, values], axis=1).astype(jnp.float32)
    ext_docs = jnp.concatenate([edge_docs, docs_own + 1])
    marker = docs_own + 1
    window_sum = jnp.zeros(values.shape, jnp.float32)
    members = jnp.zeros(values.shape, jnp.float32)
    for lag_step in range(WIDEST):
        lower_edge = reach_back - lag_step
        shifted = lax.slice_in_dim(extended, lower_edge, lower_edge + length, axis=1)
        same_doc = lax.slice_in_dim(ext_docs, lower_edge, lower_edge + length) == marker
        inside = jnp.logical_and(same_doc[None, :], lag_step < widths[:, None])
        window_sum = window_sum + jnp.where(inside, shifted, jnp.float32(0.0))
        members = members + inside.astype(jnp.float32)
    return (window_sum / members - values.astype(jnp.float32)).astype(jnp.bfloat16)


def per_device(stream, norm_gain, in_weight, out_weight, docs):
    local_rows, length = stream.shape
    pool_rows = in_weight.shape[2]
    channel = lax.axis_index("tp") * pool_rows + lax.iota(jnp.int32, pool_rows)
    widths = jnp.left_shift(jnp.int32(2), channel // (PW // GROUPS))
    residual = stream.astype(jnp.float32)
    for layer_idx in range(LAYERS):
        in_block, out_rows = (
            lax.all_gather(in_weight[layer_idx], "sp", axis=0, tiled=True),
            lax.all_gather(out_weight[layer_idx], "sp", axis=1, tiled=True),
        )
        squares = lax.psum(jnp.sum(residual * residual, axis=0), "tp")
        scaled = residual * lax.rsqrt(squares / D + 1e-06)[None, :] * norm_gain[layer_idx][:, None]
        normed = scaled.astype(jnp.bfloat16)
        pool_in = lax.dot_general(
            in_block,
            lax.all_gather(normed, "tp", axis=0, tiled=True),
            contract_rows,
            preferred_element_type=jnp.float32,
        ).astype(jnp.bfloat16)
        tail_from = length - WIDEST + 1
        edge_values, edge_docs = passed_along(
            (pool_in[:, tail_from:], docs[tail_from:] + 1), "sp", 1
        )
        pooled = trailing_pool(pool_in, docs, edge_values, edge_docs, widths)
        out_cols = lax.all_to_all(out_rows, "tp", split_axis=1, concat_axis=0, tiled=True)
        change = lax.dot_general(
            out_cols,
            lax.all_gather(pooled, "tp", axis=0, tiled=True),
            contract_rows,
            preferred_element_type=jnp.float32,
        )
        residual = residual + change
    return residual.astype(jnp.bfloat16)


HALO = 32
F32 = jnp.float32
BF16 = jnp.bfloat16


def fused_kernel(
    nsp, stream, tails, dcol, gain, inw, outw, out,
    bin_, bout, res, xn, pin, pooled, xrecv, ostage, hbuf, dbuf, gbuf, masks, invs,
    lane_sem, core_sem, sent_sem, own_sem, sx, rx, so, ro, ms, mr,
):
    nz = nsp // 4
    H = stream.shape[1] // 2
    T = H + HALO
    s, y = lax.axis_index("sp"), lax.axis_index("tp")
    c, x, z = lax.rem(s, 2), lax.rem(s // 2, 2), s // 4
    py = 1 - y
    half = PW // 2
    zw = 128
    seg = nz * zw

    def blk(k, zz, xx, cc, yy):
        l = k // 2
        if k % 2 == 0:
            row = (((l * 2 + yy) * 2 + cc) * 2 + xx) * seg + zz * zw
            return bin_.at[pl.ds(pl.multiple_of(row, zw), zw), :]
        row = (((l * 2 + cc) * 2 + xx) * 2 + yy) * half
        return bout.at[pl.ds(pl.multiple_of(row, half), half), pl.ds(pl.multiple_of(zz * zw, zw), zw)]

    def own(k):
        return (inw if k % 2 == 0 else outw).at[k // 2]

    def rcopy(src, dst, ss, rs, sp, tp):
        return pltpu.make_async_remote_copy(
            src_ref=src, dst_ref=dst, send_sem=ss, recv_sem=rs,
            device_id=(sp, tp), device_id_type=pl.DeviceIdType.MESH)

    def zat(dz):
        return lax.rem(z + dz, nz)

    def rel(dx, dy, dz):
        return (dx * 2 + dy) * nz + dz

    def place(k, dx, dy, dz):
        return blk(k, zat(dz), (x + dx) % 2 if isinstance(x, int) else lax.rem(x + dx, 2), c, lax.rem(y + dy, 2))

    def source(k, dx, dy, dz):
        return own(k) if dx == dy == dz == 0 else place(k, dx, dy, dz)

    def to_z(k, dy):
        for d in (1, nz - 1, 2) if nz == 4 else range(1, nz):
            rcopy(source(k, 0, dy, 0), place(k, 0, dy, 0), sent_sem.at[k],
                  lane_sem.at[k, rel(0, dy, nz - d)], zat(d) * 4 + x * 2 + c, y).start()

    def to_y(k, dz):
        rcopy(source(k, 0, 0, dz), place(k, 0, 0, dz), sent_sem.at[k],
              lane_sem.at[k, rel(0, 1, dz)], s, py).start()

    def to_x(k, dy, dz):
        rcopy(source(k, 0, dy, dz), place(k, 0, dy, dz), sent_sem.at[k],
              lane_sem.at[k, rel(1, dy, dz)], z * 4 + (1 - x) * 2 + c, y).start()

    def to_core(k, dx, dy, dz):
        rcopy(source(k, dx, dy, dz), place(k, dx, dy, dz), sent_sem.at[k],
              core_sem.at[k], z * 4 + x * 2 + 1 - c, y).start()

    def arrived(k, dx, dy, dz):
        rcopy(own(k), place(k, dx, dy, dz), sent_sem.at[k],
              lane_sem.at[k, rel(dx, dy, dz)], s, py).wait_recv()

    def own_sends(k):
        if k == 0:
            to_y(k, 0)
        to_z(k, 0)
        to_x(k, 0, 0)
        if k > 0:
            to_y(k, 0)
        to_core(k, 0, 0, 0)
        pltpu.make_async_copy(own(k), place(k, 0, 0, 0), own_sem.at[k]).start()

    zorder = (1, nz - 1, 2) if nz == 4 else tuple(range(1, nz))

    def z_forward(k):
        for dz in zorder:
            arrived(k, 0, 0, dz)
            if k > 0:
                to_y(k, dz)
            to_x(k, 0, dz)
            to_core(k, 0, 0, dz)

    def y_forward(k):
        if k == 0:
            arrived(k, 0, 1, 0)
            to_z(k, 1)
            to_x(k, 1, 0)
            to_core(k, 0, 1, 0)
            return
        for dz in (0,) + zorder:
            arrived(k, 0, 1, dz)
            to_x(k, 1, dz)
            to_core(k, 0, 1, dz)

    def yz_forward(k):
        for dz in zorder:
            arrived(k, 0, 1, dz)
            to_x(k, 1, dz)
            to_core(k, 0, 1, dz)

    def x_forward(k):
        order = [(0, 0)] + ([(1, 0)] if k == 0 else [])
        order += [(0, dz) for dz in zorder]
        order += [(1, dz) for dz in ((0,) if k > 0 else ()) + zorder]
        for dy, dz in order:
            arrived(k, 1, dy, dz)
            to_core(k, 1, dy, dz)

    def bulk_wait(sem, blocks):
        ref = bin_.at[pl.ds(0, blocks * zw), :]
        pltpu.make_async_copy(ref, ref, sem).wait()

    def finish(k):
        pltpu.make_async_copy(own(k), place(k, 0, 0, 0), own_sem.at[k]).wait()
        bulk_wait(core_sem.at[k], 4 * nz)

    gcopy = rcopy(gain, gbuf, ms.at[3], mr.at[3], s, py)
    t0 = rcopy(tails.at[0], hbuf.at[0], ms.at[0], mr.at[0], s, py)
    nxt = lax.rem(s + 1, nsp)
    t1 = [rcopy(tails.at[1], hbuf.at[h], ms.at[1], mr.at[h], nxt, 0) for h in (0, 1)]
    L = stream.shape[1]
    d1 = rcopy(dcol.at[pl.ds(L - HALO, HALO), :], dbuf, ms.at[2], mr.at[2], nxt, 0)
    more = s < nsp - 1
    own_sends(0)
    gcopy.start()

    @pl.when(y == 0)
    def _():
        t0.start()

    for h in (0, 1):
        @pl.when(jnp.logical_and(more, y == h))
        def _():
            t1[h].start()

    @pl.when(jnp.logical_and(more, y == 0))
    def _():
        d1.start()

    chunk = stream.shape[0] // 4
    xs = [rcopy(stream.at[pl.ds(i * chunk, chunk), pl.ds(pl.multiple_of(py * H, H), H)],
                xrecv.at[pl.ds(i * chunk, chunk), :], sx.at[i], rx.at[i], s, py) for i in range(4)]
    for cp in xs:
        cp.start()

    nb = stream.shape[0] // zw

    def col(b, h):
        cc, xx, zz = b % 2, (b // 2) % 2, h * (nz // 2) + b // 4
        return pl.multiple_of((cc * 2 + xx) * seg + zz * zw, zw)

    def turn(block):
        return block.astype(F32).T

    y_forward(0)
    own_sends(1)

    @pl.loop(0, nb)
    def _(b):
        rows = pl.ds(pl.multiple_of(b * zw, zw), zw)
        res[pl.ds(HALO, H), pl.ds(col(b, y), zw)] = turn(stream[rows, pl.ds(pl.multiple_of(y * H, H), H)])

    @pl.when(y == 1)
    def _():
        hbuf[1] = tails[0]
        dbuf[...] = dcol[pl.ds(H - HALO, HALO), :]

    @pl.when(jnp.logical_and(y == 0, s == 0))
    def _():
        hbuf[...] = jnp.zeros_like(hbuf)
        dbuf[...] = jnp.full(dbuf.shape, -1, jnp.int32)

    @pl.when(jnp.logical_or(y == 1, s > 0))
    def _():
        rcopy(tails.at[0], hbuf.at[0], ms.at[0], mr.at[0], s, py).wait_recv()

    @pl.when(jnp.logical_and(y == 0, s > 0))
    def _():
        rcopy(tails.at[0], hbuf.at[1], ms.at[0], mr.at[1], s, py).wait_recv()
        d1.wait_recv()

    gcopy.wait_recv()
    docs_all = jnp.concatenate([dbuf[...], dcol[pl.ds(pl.multiple_of(y * H, H), H), :]], axis=0)
    docs_f = docs_all.astype(F32)
    count = jnp.ones((T, 128), F32)
    for i in range(4):
        same = (pltpu.roll(docs_f, 1 << i, 0) == docs_f).astype(F32)
        masks[i] = same
        count = count + same * pltpu.roll(count, 1 << i, 0)
        invs[i] = 1.0 / count
    for h in (0, 1):
        for b in range(nb):
            cc, xx, zz = b % 2, (b // 2) % 2, h * (nz // 2) + b // 4
            at = (cc * 2 + xx) * seg + zz * zw
            res[pl.ds(0, HALO), at:at + zw] = hbuf[h, :, b * zw:(b + 1) * zw].astype(F32)

    z_forward(0)
    yz_forward(0)
    z_forward(1)
    own_sends(2)
    x_forward(0)
    per = chunk // zw
    for i in range(4):
        xs[i].wait_recv()

        @pl.loop(i * per, (i + 1) * per)
        def _(b):
            rows = pl.ds(pl.multiple_of(b * zw, zw), zw)
            res[pl.ds(HALO, H), pl.ds(col(b, py), zw)] = turn(xrecv[rows, :])

    def norm(l):
        inv = lax.rsqrt(jnp.sum(res[...] * res[...], axis=1, keepdims=True) / D + 1e-06)
        for h in (0, 1):
            g = jnp.where(y == h, gain[l], gbuf[l])
            for b in range(nb):
                cc, xx, zz = b % 2, (b // 2) % 2, h * (nz // 2) + b // 4
                at = (cc * 2 + xx) * seg + zz * zw
                xn[:, at:at + zw] = (res[:, at:at + zw] * inv * g[b:b + 1, :]).astype(BF16)

    def in_proj(l):
        for yy in (0, 1):
            w = bin_[pl.ds((l * 2 + yy) * 4 * seg, 4 * seg), :]
            acc = jnp.dot(xn[...], w, preferred_element_type=F32)
            pin[:, yy * half:(yy + 1) * half] = acc.astype(BF16).astype(F32)

    def pool():
        per_group = PW // GROUPS // 128
        for g in range(GROUPS):
            @pl.loop(0, per_group)
            def _(j):
                at = pl.ds(pl.multiple_of((g * per_group + j) * 128, 128), 128)
                v = pin[:, at]
                total = v
                for i in range(g + 1):
                    total = total + masks[i] * pltpu.roll(total, 1 << i, 0)
                pooled[:, at] = (total * invs[g] - v).astype(BF16)

    finish(0)
    norm(0)
    in_proj(0)
    y_forward(1)
    z_forward(2)
    own_sends(3)
    pool()
    x_forward(1)
    y_forward(2)
    z_forward(3)
    finish(1)

    @pl.loop(0, 4)
    def _(q):
        w = bout[pl.ds(pl.multiple_of(q * PW, PW), PW), :]
        at = pl.ds(pl.multiple_of(q * seg, seg), seg)
        res[:, at] += jnp.dot(pooled[...], w, preferred_element_type=F32)

    norm(1)
    x_forward(2)
    y_forward(3)
    finish(2)
    in_proj(1)
    pool()
    x_forward(3)
    finish(3)
    hz = nz // 2

    def last(q, h):
        cols = pl.ds(pl.multiple_of(h * hz * zw, hz * zw), hz * zw)
        w = bout[pl.ds((4 + q) * PW, PW), cols]
        at = pl.ds(pl.multiple_of(q * seg + h * hz * zw, hz * zw), hz * zw)
        r = res[pl.ds(HALO, H), at] + jnp.dot(pooled[pl.ds(HALO, H), :], w, preferred_element_type=F32)
        return r.T.astype(BF16)

    sends = []
    pending = []
    for q in range(4):
        v = last(q, py)
        for cp in pending:
            cp.start()
        pending = []
        for i in range(hz):
            b = i * 4 + (q % 2) * 2 + q // 2
            ostage[b * zw:(b + 1) * zw, :] = v[i * zw:(i + 1) * zw, :]
            pending.append(rcopy(
                ostage.at[pl.ds(b * zw, zw), :],
                out.at[pl.ds(b * zw, zw), pl.ds(pl.multiple_of(y * H, H), H)],
                so.at[b], ro.at[b], s, py))
        sends += pending
    for q in range(4):
        v = last(q, y)
        for cp in pending:
            cp.start()
        pending = []
        for i in range(hz):
            b = i * 4 + (q % 2) * 2 + q // 2
            out[b * zw:(b + 1) * zw, pl.ds(pl.multiple_of(y * H, H), H)] = v[i * zw:(i + 1) * zw, :]

    gcopy.wait_send()

    @pl.when(y == 0)
    def _():
        t0.wait_send()

    @pl.when(more)
    def _():
        t1[0].wait_send()

    @pl.when(jnp.logical_and(more, y == 0))
    def _():
        d1.wait_send()

    for cp in xs:
        cp.wait_send()
    for k in range(4):
        bulk_wait(sent_sem.at[k], 8 * nz - 1)
    for b in range(nb):
        rcopy(ostage.at[pl.ds(b * zw, zw), :],
              out.at[pl.ds(b * zw, zw), pl.ds(pl.multiple_of(py * H, H), H)],
              so.at[b], ro.at[b], s, py).wait()


def fused_device(nsp, stream, norm_gain, in_weight, out_weight, docs):
    rows, L = stream.shape
    H = L // 2
    T = H + HALO
    nz = nsp // 4
    tails = jnp.stack([stream[:, H - HALO:H].T, stream[:, L - HALO:].T])
    dcol = jnp.broadcast_to(docs[:, None], (L, 128))
    gain = norm_gain.reshape(LAYERS, rows // 128, 128)
    vmem = pl.BlockSpec(memory_space=pltpu.VMEM)
    dma = pltpu.SemaphoreType.DMA
    return pl.pallas_call(
        functools.partial(fused_kernel, nsp),
        out_shape=jax.ShapeDtypeStruct((rows, L), BF16),
        in_specs=[vmem] * 6,
        out_specs=vmem,
        scratch_shapes=[
            pltpu.VMEM((LAYERS * D * 2, PW // 2), BF16),
            pltpu.VMEM((LAYERS * PW * 4, D // 4), BF16),
            pltpu.VMEM((T, D), F32),
            pltpu.VMEM((T, D), BF16),
            pltpu.VMEM((T, PW), F32),
            pltpu.VMEM((T, PW), BF16),
            pltpu.VMEM((rows, H), BF16),
            pltpu.VMEM((rows, H), BF16),
            pltpu.VMEM((2, HALO, rows), BF16),
            pltpu.VMEM((HALO, 128), jnp.int32),
            pltpu.VMEM((LAYERS, rows // 128, 128), F32),
            pltpu.VMEM((4, T, 128), F32),
            pltpu.VMEM((4, T, 128), F32),
            dma((4, 4 * nz)), dma((4,)), dma((4,)), dma((4,)),
            dma((4,)), dma((4,)), dma((rows // 128,)), dma((rows // 128,)),
            dma((4,)), dma((4,)),
        ],
        compiler_params=pltpu.CompilerParams(has_side_effects=True, vmem_limit_bytes=60 * 1024 * 1024),
    )(stream, tails, dcol, gain, in_weight, out_weight)


def solution(mesh):
    nsp, ntp = mesh.shape["sp"], mesh.shape["tp"]
    body = per_device
    if ntp == 2 and nsp == D // 128:
        body = functools.partial(fused_device, nsp)
    return jax.shard_map(
        body,
        mesh=mesh,
        in_specs=(P("tp", "sp"), P(None, "tp"), P(None, "sp", "tp"), P(None, "tp", "sp"), P("sp")),
        out_specs=P("tp", "sp"),
        check_vma=False,
    )
```

```python
import jax
import jax.numpy as jnp
from jax import lax
from jax.experimental import pallas as pl
from jax.experimental.pallas import tpu as pltpu
from jax.sharding import PartitionSpec as P
import functools

D = 2048
PW = 1024
GROUPS = 4
WIDEST = 16
LAYERS = 2


contract_rows = (((0,), (0,)), ((), ()))


def passed_along(block, axis, distance):
    devices = range(lax.axis_size(axis))
    route = [(i - distance, i) for i in devices if i - distance in devices]
    return lax.ppermute(block, axis, route)


def trailing_pool(values, docs_own, edge_values, edge_docs, widths):
    length = values.shape[1]
    reach_back = WIDEST - 1
    extended = jnp.concatenate([edge_values, values], axis=1).astype(jnp.float32)
    ext_docs = jnp.concatenate([edge_docs, docs_own + 1])
    marker = docs_own + 1
    window_sum = jnp.zeros(values.shape, jnp.float32)
    members = jnp.zeros(values.shape, jnp.float32)
    for lag_step in range(WIDEST):
        lower_edge = reach_back - lag_step
        shifted = lax.slice_in_dim(extended, lower_edge, lower_edge + length, axis=1)
        same_doc = lax.slice_in_dim(ext_docs, lower_edge, lower_edge + length) == marker
        inside = jnp.logical_and(same_doc[None, :], lag_step < widths[:, None])
        window_sum = window_sum + jnp.where(inside, shifted, jnp.float32(0.0))
        members = members + inside.astype(jnp.float32)
    return (window_sum / members - values.astype(jnp.float32)).astype(jnp.bfloat16)


def per_device(stream, norm_gain, in_weight, out_weight, docs):
    local_rows, length = stream.shape
    pool_rows = in_weight.shape[2]
    channel = lax.axis_index("tp") * pool_rows + lax.iota(jnp.int32, pool_rows)
    widths = jnp.left_shift(jnp.int32(2), channel // (PW // GROUPS))
    residual = stream.astype(jnp.float32)
    for layer_idx in range(LAYERS):
        in_block, out_rows = (
            lax.all_gather(in_weight[layer_idx], "sp", axis=0, tiled=True),
            lax.all_gather(out_weight[layer_idx], "sp", axis=1, tiled=True),
        )
        squares = lax.psum(jnp.sum(residual * residual, axis=0), "tp")
        scaled = residual * lax.rsqrt(squares / D + 1e-06)[None, :] * norm_gain[layer_idx][:, None]
        normed = scaled.astype(jnp.bfloat16)
        pool_in = lax.dot_general(
            in_block,
            lax.all_gather(normed, "tp", axis=0, tiled=True),
            contract_rows,
            preferred_element_type=jnp.float32,
        ).astype(jnp.bfloat16)
        tail_from = length - WIDEST + 1
        edge_values, edge_docs = passed_along(
            (pool_in[:, tail_from:], docs[tail_from:] + 1), "sp", 1
        )
        pooled = trailing_pool(pool_in, docs, edge_values, edge_docs, widths)
        out_cols = lax.all_to_all(out_rows, "tp", split_axis=1, concat_axis=0, tiled=True)
        change = lax.dot_general(
            out_cols,
            lax.all_gather(pooled, "tp", axis=0, tiled=True),
            contract_rows,
            preferred_element_type=jnp.float32,
        )
        residual = residual + change
    return residual.astype(jnp.bfloat16)


HALO = 32
F32 = jnp.float32
BF16 = jnp.bfloat16


def fused_kernel(
    nsp, stream, tails, docs, gain, inw, outw, out,
    bin_, bout, res, xn, pin, pooled, xrecv, ostage, hbuf, dbuf, gbuf, masks, invs,
    lane_sem, core_sem, sent_sem, own_sem, sx, rx, so, ro, ms, mr,
):
    nz = nsp // 4
    L = stream.shape[1]
    H = L // 2
    T = H + HALO
    s, y = lax.axis_index("sp"), lax.axis_index("tp")
    c, x, z = lax.rem(s, 2), lax.rem(s // 2, 2), s // 4
    py = 1 - y
    half = PW // 2
    zw = 128
    seg = nz * zw

    def blk(k, zz, xx, cc, yy):
        l = k // 2
        if k % 2 == 0:
            row = (((l * 2 + yy) * 2 + cc) * 2 + xx) * seg + zz * zw
            return bin_.at[pl.ds(pl.multiple_of(row, zw), zw), :]
        row = (((l * 2 + cc) * 2 + xx) * 2 + yy) * half
        return bout.at[pl.ds(pl.multiple_of(row, half), half), pl.ds(pl.multiple_of(zz * zw, zw), zw)]

    def own(k):
        return (inw if k % 2 == 0 else outw).at[k // 2]

    def rcopy(src, dst, ss, rs, sp, tp):
        return pltpu.make_async_remote_copy(
            src_ref=src, dst_ref=dst, send_sem=ss, recv_sem=rs,
            device_id=(sp, tp), device_id_type=pl.DeviceIdType.MESH)

    def zat(dz):
        return lax.rem(z + dz, nz)

    def rel(dx, dy, dz):
        return (dx * 2 + dy) * nz + dz

    def place(k, dx, dy, dz):
        return blk(k, zat(dz), lax.rem(x + dx, 2), c, lax.rem(y + dy, 2))

    def source(k, dx, dy, dz):
        return own(k) if dx == dy == dz == 0 else place(k, dx, dy, dz)

    def to_z(k, dy):
        for d in (1, nz - 1, 2) if nz == 4 else range(1, nz):
            rcopy(source(k, 0, dy, 0), place(k, 0, dy, 0), sent_sem.at[k],
                  lane_sem.at[k, rel(0, dy, nz - d)], zat(d) * 4 + x * 2 + c, y).start()

    def to_y(k, dx, dz):
        rcopy(source(k, dx, 0, dz), place(k, dx, 0, dz), sent_sem.at[k],
              lane_sem.at[k, rel(dx, 1, dz)], s, py).start()

    def to_x(k, dy, dz):
        rcopy(source(k, 0, dy, dz), place(k, 0, dy, dz), sent_sem.at[k],
              lane_sem.at[k, rel(1, dy, dz)], z * 4 + (1 - x) * 2 + c, y).start()

    def to_core(k, dx, dy, dz):
        rcopy(source(k, dx, dy, dz), place(k, dx, dy, dz), sent_sem.at[k],
              core_sem.at[k, dx], z * 4 + x * 2 + 1 - c, y).start()

    def arrived(k, dx, dy, dz):
        rcopy(own(k), place(k, dx, dy, dz), sent_sem.at[k],
              lane_sem.at[k, rel(dx, dy, dz)], s, py).wait_recv()

    zorder = (1, nz - 1, 2) if nz == 4 else tuple(range(1, nz))
    x_first = {1: (1, nz - 1), 2: tuple(range(nz)), 3: ()}

    def keep_own(k):
        pltpu.make_async_copy(own(k), place(k, 0, 0, 0), own_sem.at[k]).start()

    def first_hop(k, dz):
        if dz:
            arrived(k, 0, 0, dz)
        if dz in x_first[k]:
            to_x(k, 0, dz)
            to_y(k, 0, dz)
        else:
            to_y(k, 0, dz)
            to_x(k, 0, dz)
        to_core(k, 0, 0, dz)

    def second_hop(k):
        for dz in (0,) + zorder:
            if dz in x_first[k]:
                arrived(k, 1, 0, dz)
                to_y(k, 1, dz)
                to_core(k, 1, 0, dz)
            else:
                arrived(k, 0, 1, dz)
                to_x(k, 1, dz)
                to_core(k, 0, 1, dz)

    def third_hop(k):
        for dz in (0,) + zorder:
            dx, dy = (0, 1) if dz in x_first[k] else (1, 0)
            arrived(k, dx, dy, dz)
            to_core(k, dx, dy, dz)
        for dz in (0,) + zorder:
            arrived(k, 1, 1, dz)
            to_core(k, 1, 1, dz)

    def begin0():
        to_y(0, 0, 0)
        to_z(0, 0)
        to_x(0, 0, 0)
        to_core(0, 0, 0, 0)
        keep_own(0)

    def across0():
        arrived(0, 0, 1, 0)
        to_z(0, 1)
        to_x(0, 1, 0)
        to_core(0, 0, 1, 0)

    def along0():
        for dz in zorder:
            for dy in (0, 1):
                arrived(0, 0, dy, dz)
                to_x(0, dy, dz)
                to_core(0, 0, dy, dz)

    def close0():
        for dz in (0,) + zorder:
            for dy in (0, 1):
                arrived(0, 1, dy, dz)
                to_core(0, 1, dy, dz)

    def bulk_wait(sem, blocks):
        ref = bin_.at[pl.ds(0, blocks * zw), :]
        pltpu.make_async_copy(ref, ref, sem).wait()

    def finish(k, dxs=(0, 1)):
        if 0 in dxs:
            pltpu.make_async_copy(own(k), place(k, 0, 0, 0), own_sem.at[k]).wait()
        for dx in dxs:
            bulk_wait(core_sem.at[k, dx], 2 * nz)

    gcopy = rcopy(gain, gbuf, ms.at[3], mr.at[3], s, py)
    t0 = rcopy(tails.at[0], hbuf.at[0], ms.at[0], mr.at[0], s, py)
    nxt = lax.rem(s + 1, nsp)
    t1 = [rcopy(tails.at[1], hbuf.at[h], ms.at[1], mr.at[h], nxt, 0) for h in (0, 1)]
    d1 = rcopy(docs, dbuf, ms.at[2], mr.at[2], nxt, 0)
    more = s < nsp - 1
    begin0()
    gcopy.start()

    @pl.when(y == 0)
    def _():
        t0.start()

    for h in (0, 1):
        @pl.when(jnp.logical_and(more, y == h))
        def _():
            t1[h].start()

    @pl.when(jnp.logical_and(more, y == 0))
    def _():
        d1.start()

    chunk = stream.shape[0] // 4
    xs = [rcopy(stream.at[pl.ds(i * chunk, chunk), pl.ds(pl.multiple_of(py * H, H), H)],
                xrecv.at[pl.ds(i * chunk, chunk), :], sx.at[i], rx.at[i], s, py) for i in range(4)]
    for cp in xs:
        cp.start()

    nb = stream.shape[0] // zw

    def col(b, h):
        cc, xx, zz = b % 2, (b // 2) % 2, h * (nz // 2) + b // 4
        return pl.multiple_of((cc * 2 + xx) * seg + zz * zw, zw)

    def turn(block):
        return block.astype(F32).T

    across0()
    for k in (1, 2, 3):
        to_z(k, 0)
        keep_own(k)

    @pl.loop(0, nb)
    def _(b):
        rows = pl.ds(pl.multiple_of(b * zw, zw), zw)
        res[pl.ds(HALO, H), pl.ds(col(b, y), zw)] = turn(stream[rows, pl.ds(pl.multiple_of(y * H, H), H)])

    @pl.when(y == 1)
    def _():
        hbuf[1] = tails[0]
        dbuf[L // zw - 1:L // zw] = docs[H // zw - 1:H // zw]

    @pl.when(jnp.logical_and(y == 0, s == 0))
    def _():
        hbuf[...] = jnp.zeros_like(hbuf)
        dbuf[...] = jnp.full(dbuf.shape, -1, jnp.int32)

    @pl.when(jnp.logical_or(y == 1, s > 0))
    def _():
        rcopy(tails.at[0], hbuf.at[0], ms.at[0], mr.at[0], s, py).wait_recv()

    @pl.when(jnp.logical_and(y == 0, s > 0))
    def _():
        rcopy(tails.at[0], hbuf.at[1], ms.at[0], mr.at[1], s, py).wait_recv()
        d1.wait_recv()

    gcopy.wait_recv()

    def upright(row):
        return jnp.broadcast_to(row.astype(F32), (zw, zw)).T

    docs_f = jnp.concatenate(
        [upright(dbuf[L // zw - 1:L // zw])[zw - HALO:]]
        + [upright(jnp.where(y == 0, docs[i:i + 1], docs[H // zw + i:H // zw + i + 1])) for i in range(H // zw)],
        axis=0)
    count = jnp.ones((T, 128), F32)
    for i in range(4):
        same = (pltpu.roll(docs_f, 1 << i, 0) == docs_f).astype(F32)
        masks[i] = same
        count = count + same * pltpu.roll(count, 1 << i, 0)
        invs[i] = 1.0 / count
    for h in (0, 1):
        for b in range(nb):
            cc, xx, zz = b % 2, (b // 2) % 2, h * (nz // 2) + b // 4
            at = (cc * 2 + xx) * seg + zz * zw
            res[pl.ds(0, HALO), at:at + zw] = hbuf[h, :, b * zw:(b + 1) * zw].astype(F32)

    along0()
    for dz in (0,) + zorder:
        first_hop(1, dz)
    close0()
    per = chunk // zw
    for i in range(4):
        xs[i].wait_recv()

        @pl.loop(i * per, (i + 1) * per)
        def _(b):
            rows = pl.ds(pl.multiple_of(b * zw, zw), zw)
            res[pl.ds(HALO, H), pl.ds(col(b, py), zw)] = turn(xrecv[rows, :])

    def norm(l):
        inv = lax.rsqrt(jnp.sum(res[...] * res[...], axis=1, keepdims=True) / D + 1e-06)
        for h in (0, 1):
            g = jnp.where(y == h, gain[l], gbuf[l])
            for b in range(nb):
                cc, xx, zz = b % 2, (b // 2) % 2, h * (nz // 2) + b // 4
                at = (cc * 2 + xx) * seg + zz * zw
                xn[:, at:at + zw] = (res[:, at:at + zw] * inv * g[b:b + 1, :]).astype(BF16)

    def in_proj(l):
        for yy in (0, 1):
            w = bin_[pl.ds((l * 2 + yy) * 4 * seg, 4 * seg), :]
            acc = jnp.dot(xn[...], w, preferred_element_type=F32)
            pin[:, yy * half:(yy + 1) * half] = acc.astype(BF16).astype(F32)

    def pool():
        per_group = PW // GROUPS // 128
        for g in range(GROUPS):
            @pl.loop(0, per_group)
            def _(j):
                at = pl.ds(pl.multiple_of((g * per_group + j) * 128, 128), 128)
                v = pin[:, at]
                total = v
                for i in range(g + 1):
                    total = total + masks[i] * pltpu.roll(total, 1 << i, 0)
                pooled[:, at] = (total * invs[g] - v).astype(BF16)

    for dz in (0,) + zorder:
        first_hop(2, dz)
    finish(0)
    norm(0)
    in_proj(0)
    second_hop(1)
    for dz in (0,) + zorder:
        first_hop(3, dz)
    pool()
    second_hop(2)
    third_hop(1)
    finish(1)

    @pl.loop(0, 4)
    def _(q):
        w = bout[pl.ds(pl.multiple_of(q * PW, PW), PW), :]
        at = pl.ds(pl.multiple_of(q * seg, seg), seg)
        res[:, at] += jnp.dot(pooled[...], w, preferred_element_type=F32)

    norm(1)
    second_hop(3)
    third_hop(2)
    finish(2)
    in_proj(1)
    pool()
    finish(3, (0,))
    hz = nz // 2

    def last(q, h):
        cols = pl.ds(pl.multiple_of(h * hz * zw, hz * zw), hz * zw)
        w = bout[pl.ds(pl.multiple_of((4 + q) * PW, PW), PW), cols]
        at = pl.ds(pl.multiple_of(q * seg + h * hz * zw, hz * zw), hz * zw)
        r = res[pl.ds(HALO, H), at] + jnp.dot(pooled[pl.ds(HALO, H), :], w, preferred_element_type=F32)
        return r.T.astype(BF16)

    def part(dx, dc):
        return lax.rem(c + dc, 2), lax.rem(x + dx, 2)

    def outward(dx, dc):
        cc, xx = part(dx, dc)
        v = last(cc * 2 + xx, py)
        for i in range(hz):
            b = i * 4 + xx * 2 + cc
            rows = pl.ds(pl.multiple_of(b * zw, zw), zw)
            ostage[rows, :] = v[i * zw:(i + 1) * zw, :]
        for i in range(hz):
            b = i * 4 + xx * 2 + cc
            rows = pl.ds(pl.multiple_of(b * zw, zw), zw)
            rcopy(ostage.at[rows, :], out.at[rows, pl.ds(pl.multiple_of(y * H, H), H)],
                  so.at[b], ro.at[b], s, py).start()

    outward(0, 0)
    outward(0, 1)
    third_hop(3)
    finish(3, (1,))
    outward(1, 0)
    outward(1, 1)
    for dx in (0, 1):
        for dc in (0, 1):
            cc, xx = part(dx, dc)
            v = last(cc * 2 + xx, y)
            for i in range(hz):
                rows = pl.ds(pl.multiple_of((i * 4 + xx * 2 + cc) * zw, zw), zw)
                out[rows, pl.ds(pl.multiple_of(y * H, H), H)] = v[i * zw:(i + 1) * zw, :]

    gcopy.wait_send()

    @pl.when(y == 0)
    def _():
        t0.wait_send()

    @pl.when(more)
    def _():
        t1[0].wait_send()

    @pl.when(jnp.logical_and(more, y == 0))
    def _():
        d1.wait_send()

    for cp in xs:
        cp.wait_send()
    for k in range(4):
        bulk_wait(sent_sem.at[k], 8 * nz - 1)
    for b in range(nb):
        rcopy(ostage.at[pl.ds(b * zw, zw), :],
              out.at[pl.ds(b * zw, zw), pl.ds(pl.multiple_of(py * H, H), H)],
              so.at[b], ro.at[b], s, py).wait()


def fused_device(nsp, stream, norm_gain, in_weight, out_weight, docs):
    rows, L = stream.shape
    H = L // 2
    T = H + HALO
    nz = nsp // 4
    tails = jnp.stack([stream[:, H - HALO:H].T, stream[:, L - HALO:].T])
    gain = norm_gain.reshape(LAYERS, rows // 128, 128)
    vmem = pl.BlockSpec(memory_space=pltpu.VMEM)
    dma = pltpu.SemaphoreType.DMA
    return pl.pallas_call(
        functools.partial(fused_kernel, nsp),
        out_shape=jax.ShapeDtypeStruct((rows, L), BF16),
        in_specs=[vmem] * 6,
        out_specs=vmem,
        scratch_shapes=[
            pltpu.VMEM((LAYERS * D * 2, PW // 2), BF16),
            pltpu.VMEM((LAYERS * PW * 4, D // 4), BF16),
            pltpu.VMEM((T, D), F32),
            pltpu.VMEM((T, D), BF16),
            pltpu.VMEM((T, PW), F32),
            pltpu.VMEM((T, PW), BF16),
            pltpu.VMEM((rows, H), BF16),
            pltpu.VMEM((rows, H), BF16),
            pltpu.VMEM((2, HALO, rows), BF16),
            pltpu.VMEM((L // 128, 128), jnp.int32),
            pltpu.VMEM((LAYERS, rows // 128, 128), F32),
            pltpu.VMEM((4, T, 128), F32),
            pltpu.VMEM((4, T, 128), F32),
            dma((4, 4 * nz)), dma((4, 2)), dma((4,)), dma((4,)),
            dma((4,)), dma((4,)), dma((rows // 128,)), dma((rows // 128,)),
            dma((4,)), dma((4,)),
        ],
        compiler_params=pltpu.CompilerParams(has_side_effects=True, vmem_limit_bytes=60 * 1024 * 1024),
    )(stream, tails, docs.reshape(L // 128, 128), gain, in_weight, out_weight)


def solution(mesh):
    nsp, ntp = mesh.shape["sp"], mesh.shape["tp"]
    body = per_device
    if ntp == 2 and nsp == D // 128:
        body = functools.partial(fused_device, nsp)
    return jax.shard_map(
        body,
        mesh=mesh,
        in_specs=(P("tp", "sp"), P(None, "tp"), P(None, "sp", "tp"), P(None, "tp", "sp"), P("sp")),
        out_specs=P("tp", "sp"),
        check_vma=False,
    )
```
